32 devices in a mesh: ep: 8 (over z, core), tp: 4 (over y, x).
Axes of the slice: x: 2, y: 2, z: 4, core: 2. Of those that a mesh axis runs over, the one named last changes fastest.
Arguments:
- tokens: bfloat16 [1024, 4096], P('ep', 'tp'), may hold values from -6 to 6
- out_grad: bfloat16 [1024, 4096], P('ep', 'tp'), may hold values from -1.5 to 1.5
- routes: int32 [1024, 2], P('ep'), may hold values from 0 to 7, all different within a row; in each aligned block of 128 rows (0 to 127, 128 to 255, ...) at most 40 rows name the same one
- route_weights: float32 [1024, 2], P('ep'), may hold values from 0.2 to 1.2
- gate_proj: bfloat16 [8, 1024, 4096], P('ep', 'tp'), may hold values from -0.09375 to 0.09375
- up_proj: bfloat16 [8, 1024, 4096], P('ep', 'tp'), may hold values from -0.09375 to 0.09375
- down_proj: bfloat16 [8, 1024, 4096], P('ep', 'tp'), may hold values from -0.1875 to 0.1875
- shared_hidden: bfloat16 [1024, 1024], P('ep'), may hold values from -6 to 6
Outputs:
- token_grad: bfloat16 [1024, 4096], P('ep', 'tp')
- weight_grad: float32 [1024, 2], P('ep')
- gate_grad: bfloat16 [8, 1024, 4096], P('ep', 'tp')
- up_grad: bfloat16 [8, 1024, 4096], P('ep', 'tp')
- down_grad: bfloat16 [8, 1024, 4096], P('ep', 'tp')
- shared_grad: float32 [1024, 4096], P('ep', 'tp')
The draws below stay inside these ranges and needn't reach their ends.
Inputs may be any that keep to these rules, and one draw needn't show every extreme that they name: Within each block of 128 consecutive tokens, no expert is named by more than 40 routes, and in some blocks one expert is named by exactly 40. The 2 experts of one token differ.
All inputs are finite; a program needn't handle non-finite values.
Results may differ from the reference program's by a relative error of at most 0.0065.
Values may be sent and summed in bfloat16 or wider, within the bound.
A program may use at most 64 MiB of HBM per device.

```python
import math
import jax
import jax.numpy as jnp
import numpy as np
from jax import lax

D = 4096
FE = 1024
FS = 1024
TOP = 2
TOK_DEV = 128
EXPERTS = 8
TOKENS = 1024
CAP = 40
N_EP = 8
N_TP = 4


def strengthened(array, key, source, target, parts, factor):
    owner, partner = [(jnp.arange(array.shape[position]) // (array.shape[position] // parts)).reshape([-1 if axis == position else 1 for axis in range(array.ndim)]) for position in (source, target)]
    chosen = jax.random.permutation(key, parts)[partner]
    strong = (owner == chosen) | (owner == (partner + parts // 2) % parts)
    return jnp.where(strong, factor * array, array)


def steps_of(rng, extent, split, smallest, top_value):
    def one(axis_at, parts):
        steps = jax.random.uniform(jax.random.fold_in(jax.random.fold_in(rng, 6), axis_at), (parts,), jnp.float32, smallest / len(split), top_value / len(split))
        return jnp.repeat(jnp.exp(steps), extent[axis_at] // parts).reshape((-1,) + (1,) * (len(extent) - axis_at - 1))

    gain = one(*split[0])
    for cut in split[1:]:
        gain = gain * one(*cut)
    return gain


def shared_out(rng, own, number, rows, number_of, top, bound, slope):
    sequence = jax.random.permutation(rng, number_of)
    heavy_load, common = portions_of(number_of, rows * top, bound, slope, True), portions_of(number_of, rows * top, bound, slope, False)
    places = jnp.arange(number_of)

    def named(lengths, rotation):
        used = int((lengths > 0).sum())
        fixed = max(1, used // 4)
        moved = fixed + (places - fixed + rotation * (used - fixed)) % max(1, number_of - fixed)
        return jnp.zeros((number_of,), jnp.int32).at[sequence[jnp.where(places < fixed, places, moved)]].set(jnp.asarray(lengths, jnp.int32))

    lengths = jnp.where(number % 4 == 0, named(heavy_load, number // 4), named(common, number - number // 4 - 1))
    mixed = jax.random.permutation(jax.random.fold_in(own, 3), number_of)
    source_of, taker = mixed[0:number_of // 2 * 2:2], mixed[1:number_of // 2 * 2:2]
    room = jnp.minimum(lengths[source_of] - 1, bound - lengths[taker]) // 2
    room = jnp.where((source_of == sequence[0]) | (taker == sequence[0]) | (lengths[taker] == 0), 0, jnp.maximum(room, 0))
    moved = jax.random.randint(jax.random.fold_in(own, 4), (number_of // 2,), 0, 1 << 20) % (room + 1)
    lengths = lengths.at[source_of].add(-moved).at[taker].add(moved)
    members = jnp.searchsorted(jnp.cumsum(lengths), jnp.arange(rows * top), side="right").astype(jnp.int32)
    table = members.reshape(top, rows).T
    table = table[jax.random.permutation(jax.random.fold_in(own, 1), rows)]
    rotation = jax.random.randint(jax.random.fold_in(own, 2), (rows, 1), 0, top)
    return jnp.take_along_axis(table, (jnp.arange(top)[None, :] + rotation) % top, axis=1)


def portions_of(amount, total, bound, slope, full):
    loads = [(1 << 20) // math.isqrt(grade ** slope) + 1 for grade in range(1, amount + 1)]
    largest = bound if full else min(bound, max(-(-total // amount), total * loads[0] // sum(loads)))
    least = 1 if total - largest >= amount - 1 else 0
    holding, spare = [largest] + [least] * (amount - 1), total - largest - least * (amount - 1)
    while spare > 0:
        free = [i for i in range(1, amount) if holding[i] < largest] or [i for i in range(1, amount) if holding[i] < bound]
        mass, remaining = sum([loads[i] for i in free]), spare
        for i in free:
            addition = min(bound - holding[i], max(1, remaining * loads[i] // mass), spare)
            holding[i] = holding[i] + addition
            spare = spare - addition
    return np.array(holding)


def bell_draw(rng, extent, spread, bound, split=(), held_as=jnp.bfloat16):
    level = steps_of(rng, extent, split, -0.22, 0.18) if split else 1.0
    array = jax.random.normal(rng, extent, jnp.float32) * spread * level
    return jnp.minimum(jnp.maximum(array, -bound), bound).astype(held_as)


def gaussian_with(key, extent, scale, most, cuts, heavy, kind=jnp.bfloat16):
    result = scale * jax.random.normal(key, extent, jnp.float32)
    if cuts:
        result = result * steps_of(key, extent, cuts, -0.22, 0.18)
    return jnp.clip(strengthened(result, jax.random.fold_in(key, 3), *heavy), -most, most).astype(kind)


def setup_inputs(seed: int = 0) -> dict:
    streams_of = jax.random.split(jax.random.key(seed), 9)
    tokens = bell_draw(streams_of[0], (TOKENS, D), 1.0, 6.0, ((0, 8), (1, 4)))
    out_grad = bell_draw(streams_of[1], (TOKENS, D), 0.25, 1.5, ((0, 8), (1, 4)))
    routes_keys = jax.random.split(jax.random.fold_in(streams_of[2], 1), TOKENS // TOK_DEV)
    routes_turns = jax.random.permutation(jax.random.fold_in(streams_of[2], 3), TOKENS // TOK_DEV)
    routes = jax.vmap(lambda own, number: shared_out(jax.random.fold_in(streams_of[2], 2), own, number, TOK_DEV, EXPERTS, TOP, CAP, 2))(routes_keys, routes_turns).reshape((TOKENS, TOP))
    route_weights = jnp.clip(0.2 + 1 * jax.random.uniform(streams_of[3], (TOKENS, TOP), jnp.float32) ** steps_of(streams_of[3], (TOKENS, TOP), ((0, 8),), -0.2, 0.2), 0.2, 1.2)
    gate_proj = bell_draw(streams_of[4], (EXPERTS, FE, D), D ** -0.5, 0.09375, ((0, 8), (1, 4)))
    up_proj = bell_draw(streams_of[5], (EXPERTS, FE, D), D ** -0.5, 0.09375, ((0, 8), (1, 4)))
    down_proj = bell_draw(streams_of[6], (EXPERTS, FE, D), FE ** -0.5, 0.1875, ((0, 8), (1, 4)))
    shared_hidden = gaussian_with(streams_of[7], (TOKENS, FS), 1.0, 6.0, ((0, 8),), (0, 1, 8, 2.0))
    return {"tokens": tokens, "out_grad": out_grad, "routes": routes, "route_weights": route_weights, "gate_proj": gate_proj, "up_proj": up_proj, "down_proj": down_proj, "shared_hidden": shared_hidden}


def reference(tokens, out_grad, routes, route_weights, gate_proj, up_proj, down_proj, shared_hidden):
    block_routes = TOK_DEV * TOP
    expert_rows = N_EP * CAP
    flat_routes = routes.reshape(N_EP, block_routes)
    expert_ids = jnp.arange(EXPERTS, dtype=jnp.int32)
    onehot = (flat_routes[:, :, None] == expert_ids[None, None, :]).astype(jnp.int32)
    slot_rank = jnp.sum((jnp.cumsum(onehot, axis=1) - 1) * onehot, axis=2)
    block_ids = jnp.arange(N_EP, dtype=jnp.int32)[:, None]
    slot_index = (flat_routes * expert_rows + block_ids * CAP + slot_rank).reshape(-1).astype(jnp.int32)
    route_ids = jnp.arange(TOKENS * TOP, dtype=jnp.int32)
    route_of_slot = jnp.full((EXPERTS * expert_rows,), -1, jnp.int32).at[slot_index].set(route_ids)
    filled = route_of_slot >= 0
    safe_route = jnp.maximum(route_of_slot, 0).astype(jnp.int32)
    token_of_slot = (safe_route // TOP).astype(jnp.int32)
    weight_b = lax.optimization_barrier(route_weights.reshape(-1).astype(jnp.bfloat16)).astype(jnp.float32)
    slot_weight = jnp.where(filled, weight_b[safe_route], jnp.zeros((), jnp.float32))
    zero_value = jnp.zeros((), jnp.bfloat16)
    slot_tokens = jnp.where(filled[:, None], tokens[token_of_slot], zero_value).reshape(EXPERTS, expert_rows, D)
    slot_grads = jnp.where(filled[:, None], out_grad[token_of_slot], zero_value).reshape(EXPERTS, expert_rows, D)
    slot_scale = slot_weight.reshape(EXPERTS, expert_rows)
    block_width = FE // N_TP
    contract_features = (((1,), (1,)), ((), ()))
    contract_rows = (((0,), (0,)), ((), ()))

    def one_expert(operands):
        rows_in, grads_in, scale, gate_matrix, up_matrix, down_matrix = operands
        pre_gate = lax.dot_general(rows_in, gate_matrix, contract_features, preferred_element_type=jnp.float32)
        pre_up = lax.dot_general(rows_in, up_matrix, contract_features, preferred_element_type=jnp.float32)
        squash = jax.nn.sigmoid(pre_gate)
        activated = pre_gate * squash
        hidden = lax.optimization_barrier((activated * pre_up).astype(jnp.bfloat16))
        back_grad = lax.dot_general(grads_in, down_matrix, contract_features,
                                    preferred_element_type=jnp.float32)
        products = jnp.sum(hidden.astype(jnp.float32) * back_grad, axis=1)
        hidden_grad = scale[:, None] * back_grad
        scaled_hidden = (scale[:, None] * hidden.astype(jnp.float32)).astype(jnp.bfloat16)
        gate_delta = (hidden_grad * pre_up * squash * (1.0 + pre_gate * (1.0 - squash))).astype(jnp.bfloat16)
        up_delta = (hidden_grad * activated).astype(jnp.bfloat16)
        gate_part = lax.dot_general(gate_delta, rows_in, contract_rows,
                                    preferred_element_type=jnp.float32).astype(jnp.bfloat16)
        up_part = lax.dot_general(up_delta, rows_in, contract_rows,
                                  preferred_element_type=jnp.float32).astype(jnp.bfloat16)
        down_part = lax.dot_general(scaled_hidden, grads_in, contract_rows,
                                    preferred_element_type=jnp.float32).astype(jnp.bfloat16)
        gate_blocks = gate_delta.astype(jnp.float32).reshape(-1, N_TP, block_width)
        up_blocks = up_delta.astype(jnp.float32).reshape(-1, N_TP, block_width)
        gate_weights = gate_matrix.astype(jnp.float32).reshape(N_TP, block_width, D)
        up_weights = up_matrix.astype(jnp.float32).reshape(N_TP, block_width, D)
        block_part = jnp.einsum('rtf,tfd->trd', gate_blocks, gate_weights) + jnp.einsum('rtf,tfd->trd', up_blocks, up_weights)
        block_part = lax.optimization_barrier(block_part.astype(jnp.bfloat16)).astype(jnp.float32)
        return jnp.sum(block_part, axis=0), products, gate_part, up_part, down_part

    route_rows, products, gate_grad, up_grad, down_grad = lax.map(
        one_expert, (slot_tokens, slot_grads, slot_scale, gate_proj, up_proj, down_proj))
    route_rows = route_rows.reshape(EXPERTS * expert_rows, D)
    products = products.reshape(-1)
    token_grad = jnp.sum(route_rows[slot_index].reshape(TOKENS, TOP, D), axis=1).astype(jnp.bfloat16)
    weight_grad = products[slot_index].reshape(TOKENS, TOP)
    shared_grad = lax.dot_general(shared_hidden, out_grad, (((0,), (0,)), ((), ())),
                                  preferred_element_type=jnp.float32)
    return token_grad, weight_grad, gate_grad, up_grad, down_grad, shared_grad
```

```python
import jax
import jax.numpy as jnp
from jax import lax
from jax.sharding import PartitionSpec as P

LANES = 128


def slot_masks(routes, num_experts, capacity):
    tok_rows, per_token = routes.shape
    expert_ids = lax.broadcasted_iota(jnp.int32, (tok_rows, num_experts), 1)
    chosen = [routes[:, k : k + 1] == expert_ids for k in range(per_token)]
    named = sum(c.astype(jnp.bfloat16) for c in chosen)
    before = (
        lax.broadcasted_iota(jnp.int32, (tok_rows, tok_rows), 1)
        < lax.broadcasted_iota(jnp.int32, (tok_rows, tok_rows), 0)
    ).astype(jnp.bfloat16)
    rank = jnp.dot(before, named, preferred_element_type=jnp.float32)
    slots = lax.broadcasted_iota(jnp.int32, (num_experts * capacity, tok_rows), 0)
    masks = []
    for k in range(per_token):
        own_rank = jnp.sum(jnp.where(chosen[k], rank, 0.0), axis=1).astype(jnp.int32)
        masks.append(slots == (routes[:, k] * capacity + own_rank)[None, :])
    return masks


def split_columns(values, width):
    high = values.astype(jnp.bfloat16)
    low = (values - high.astype(jnp.float32)).astype(jnp.bfloat16)
    pair = jnp.stack([high, low], axis=-1)
    return jnp.pad(pair, [(0, 0)] * values.ndim + [(0, width - 2)])


def local(tokens, out_grad, routes, route_weights, gate_proj, up_proj, down_proj, shared_hidden):
    ep_count = lax.axis_size("ep")
    tp_count = lax.axis_size("tp")
    local_experts = gate_proj.shape[0]
    num_experts = local_experts * ep_count
    tok_rows, per_token = routes.shape
    width = tokens.shape[1]
    capacity = max(2, 5 * tok_rows * per_token // (4 * num_experts))
    slot_count = num_experts * capacity
    masks = slot_masks(routes, num_experts, capacity)
    picks = [m.astype(jnp.bfloat16) for m in masks]
    pick = sum(picks)
    weight_b = route_weights.astype(jnp.bfloat16).astype(jnp.float32)
    slot_weight = sum(
        jnp.sum(jnp.where(masks[k], weight_b[:, k][None, :], 0.0), axis=1)
        for k in range(per_token)
    ).astype(jnp.bfloat16)
    sent = jnp.concatenate(
        [
            jnp.dot(pick, tokens, preferred_element_type=jnp.float32).astype(jnp.bfloat16),
            jnp.dot(pick, out_grad, preferred_element_type=jnp.float32).astype(jnp.bfloat16),
            jnp.pad(slot_weight[:, None], ((0, 0), (0, LANES - 1))),
        ],
        axis=1,
    ).reshape(ep_count, local_experts * capacity, 2 * width + LANES)
    came = lax.all_to_all(sent, "ep", split_axis=0, concat_axis=0, tiled=True)
    came = came.reshape(ep_count, local_experts, capacity, -1).transpose(1, 0, 2, 3)
    came = came.reshape(local_experts, ep_count * capacity, -1)
    slot_scale = came[:, :, 2 * width].astype(jnp.float32)
    rows_in = lax.all_gather(came[:, :, :width], "tp", axis=2, tiled=True)
    grads_in = lax.all_gather(came[:, :, width : 2 * width], "tp", axis=2, tiled=True)
    pre_gate = jnp.einsum("lrd,lfd->lrf", rows_in, gate_proj, preferred_element_type=jnp.float32)
    pre_up = jnp.einsum("lrd,lfd->lrf", rows_in, up_proj, preferred_element_type=jnp.float32)
    squash = jax.nn.sigmoid(pre_gate)
    activated = pre_gate * squash
    hidden = (activated * pre_up).astype(jnp.bfloat16)
    back_grad = jnp.einsum("lrd,lfd->lrf", grads_in, down_proj, preferred_element_type=jnp.float32)
    products = jnp.sum(hidden.astype(jnp.float32) * back_grad, axis=2)
    hidden_grad = slot_scale[:, :, None] * back_grad
    scaled_hidden = (slot_scale[:, :, None] * hidden.astype(jnp.float32)).astype(jnp.bfloat16)
    gate_delta = (hidden_grad * pre_up * squash * (1.0 + pre_gate * (1.0 - squash))).astype(
        jnp.bfloat16
    )
    up_delta = (hidden_grad * activated).astype(jnp.bfloat16)
    sides = split_columns(products, LANES)
    blocks = []
    for t in range(tp_count):
        cut = slice(t * width, (t + 1) * width)
        part = jnp.einsum(
            "lrf,lfd->lrd", gate_delta, gate_proj[:, :, cut], preferred_element_type=jnp.float32
        ) + jnp.einsum(
            "lrf,lfd->lrd", up_delta, up_proj[:, :, cut], preferred_element_type=jnp.float32
        )
        blocks.append(jnp.concatenate([part.astype(jnp.bfloat16), sides], axis=2))
    blocks = jnp.stack(blocks)
    parts = lax.all_to_all(blocks, "tp", split_axis=0, concat_axis=0, tiled=True)
    parts = parts.astype(jnp.float32)
    summed = jnp.sum(parts[..., :width], axis=0).astype(jnp.bfloat16)
    total = jnp.sum(parts[..., width] + parts[..., width + 1], axis=0)
    back = jnp.concatenate([summed, split_columns(total, LANES)], axis=2)
    back = back.reshape(local_experts, ep_count, capacity, -1).transpose(1, 0, 2, 3)
    back = back.reshape(ep_count, local_experts * capacity, -1)
    slot_rows = lax.all_to_all(back, "ep", split_axis=0, concat_axis=0, tiled=True)
    slot_rows = slot_rows.reshape(slot_count, -1)
    gate_grad = jnp.einsum(
        "lrf,lrd->lfd", gate_delta, rows_in, preferred_element_type=jnp.float32
    ).astype(jnp.bfloat16)
    up_grad = jnp.einsum(
        "lrf,lrd->lfd", up_delta, rows_in, preferred_element_type=jnp.float32
    ).astype(jnp.bfloat16)
    down_grad = jnp.einsum(
        "lrf,lrd->lfd", scaled_hidden, grads_in, preferred_element_type=jnp.float32
    ).astype(jnp.bfloat16)
    contract_slots = (((0,), (0,)), ((), ()))
    token_grad = lax.dot_general(
        pick, slot_rows[:, :width], contract_slots, preferred_element_type=jnp.float32
    ).astype(jnp.bfloat16)
    tail = slot_rows[:, width:].astype(jnp.float32)
    slot_product = (tail[:, 0] + tail[:, 1])[:, None]
    weight_grad = jnp.stack(
        [jnp.sum(jnp.where(m, slot_product, 0.0), axis=0) for m in masks], axis=1
    )
    shared_grad = lax.psum_scatter(
        lax.dot_general(
            shared_hidden, out_grad, (((0,), (0,)), ((), ())), preferred_element_type=jnp.float32
        ),
        "ep",
        scatter_dimension=0,
        tiled=True,
    )
    return (token_grad, weight_grad, gate_grad, up_grad, down_grad, shared_grad)


def solution(mesh):
    return jax.shard_map(
        local,
        mesh=mesh,
        in_specs=(
            P("ep", "tp"),
            P("ep", "tp"),
            P("ep", None),
            P("ep", None),
            P("ep", "tp", None),
            P("ep", "tp", None),
            P("ep", "tp", None),
            P("ep", None),
        ),
        out_specs=(
            P("ep", "tp"),
            P("ep", None),
            P("ep", "tp", None),
            P("ep", "tp", None),
            P("ep", "tp", None),
            P("ep", "tp"),
        ),
        check_vma=False,
    )
```

```python
import functools

import jax
import jax.numpy as jnp
from jax import lax
from jax.experimental import pallas as pl
from jax.experimental.pallas import tpu as pltpu
from jax.sharding import PartitionSpec as P

LANES = 128
MESH = pl.DeviceIdType.MESH


def greet(me, ep_count, mine, tp_count):
    barrier = pltpu.get_barrier_semaphore()
    for d in range(1, ep_count):
        pl.semaphore_signal(barrier, inc=1, device_id=(me ^ d, mine), device_id_type=MESH)
    for d in range(1, tp_count):
        pl.semaphore_signal(barrier, inc=1, device_id=(me, mine ^ d), device_id_type=MESH)
    pl.semaphore_wait(barrier, ep_count + tp_count - 2)


def remote(src, dst, send_sem, recv_sem, target):
    return pltpu.make_async_remote_copy(
        src_ref=src,
        dst_ref=dst,
        send_sem=send_sem,
        recv_sem=recv_sem,
        device_id=target,
        device_id_type=MESH,
    )


def dispatch_kernel(
    ep_count, tp_count, width,
    sent, grads, cols, full, all_grads, all_cols,
    ep_send, ep_recv, tp_send, tp_recv, col_send, col_recv,
    up_send, down_send, side_send, shard_recv,
):
    me, mine = lax.axis_index("ep"), lax.axis_index("tp")
    chips, z, core = ep_count // 2, me // 2, me % 2
    partner = me + 1 - 2 * core
    relay = tp_count == 4
    total = sent.shape[-1]
    halves = [(0, width), (width, total - width)] if relay else [(0, total)]
    greet(me, ep_count, mine, tp_count)
    order = sorted(range(1, ep_count), key=lambda d: (d.bit_count(), d))

    def ep_copy(d):
        return remote(
            sent.at[me ^ d], full.at[mine, me], ep_send.at[d], ep_recv.at[d], (me ^ d, mine)
        )

    def col_copy(d):
        return remote(
            cols.at[me ^ d], all_cols.at[me], col_send.at[d], col_recv.at[d], (me ^ d, mine)
        )

    def tp_copy(owner, d, via, h):
        start, size = halves[h]
        j = me ^ d
        cut = pl.ds(start, size)
        if owner == 0 and d == 0:
            src = sent.at[me, :, cut]
        else:
            src = full.at[mine ^ owner, j, :, cut]
        lane = owner ^ via
        return remote(
            src,
            full.at[mine ^ owner, j, :, cut],
            tp_send.at[lane, d, h],
            tp_recv.at[lane, d, h],
            (me, mine ^ via),
        )

    def shard_copy(shard, step, target, sem):
        src = grads if step == 0 else all_grads.at[shard]
        return remote(src, all_grads.at[shard], sem, shard_recv.at[shard], (target, mine))

    def guarded(flag, action):
        pl.when(flag)(action)

    def shard_step(step, waiting=False):
        act = (lambda c: c.wait_send()) if waiting else (lambda c: c.start())
        low, high = me - 2 * step, me + 2 * step

        def go_up():
            act(shard_copy(low, step, me + 2, up_send.at[step]))

        def go_down():
            act(shard_copy(high, step, me - 2, down_send.at[step]))

        def from_low():
            if step and not waiting:
                shard_copy(low, step, partner, side_send.at[0, step]).wait_recv()
            guarded(z + 1 < chips, go_up)
            act(shard_copy(low, step, partner, side_send.at[0, step]))

        def from_high():
            if not waiting:
                shard_copy(high, step, partner, side_send.at[1, step]).wait_recv()
            guarded(z > 0, go_down)
            act(shard_copy(high, step, partner, side_send.at[1, step]))

        if step == 0:
            from_low()
            guarded(z > 0, go_down)
        else:
            guarded(z - step >= 0, from_low)
            guarded(z + step < chips, from_high)

    for d in order:
        ep_copy(d).start()
    shard_step(0)
    for d in order:
        col_copy(d).start()
    full[mine, me] = sent[me]
    all_grads[me] = grads[...]
    all_cols[me] = cols[me]

    def pass_on(d):
        if relay:
            tp_copy(1, d, 0, 0).wait_recv()
            tp_copy(1, d, 2, 0).start()
            tp_copy(2, d, 0, 1).wait_recv()
            tp_copy(2, d, 1, 1).start()

    steps = [0] + order
    shard_at = {ep_count - chips + s: s for s in range(1, chips)}
    for k, d in enumerate(steps):
        if d:
            ep_copy(d).wait_recv()
        for via in (1, 2) if relay else range(1, tp_count):
            for h in range(len(halves)):
                tp_copy(0, d, via, h).start()
        if k:
            pass_on(steps[k - 1])
        if k in shard_at:
            shard_step(shard_at[k])
    pass_on(steps[-1])
    for s in range(1, chips):
        if s not in shard_at.values():
            shard_step(s)
    for d in steps:
        for via in range(1, tp_count):
            for h in range(len(halves)):
                done = not relay or via == 3 or (via, h) not in ((1, 0), (2, 1))
                if done:
                    tp_copy(via, d, 0, h).wait_recv()
    for zz in range(chips):
        shard_copy(2 * zz + 1 - core, 1, partner, side_send.at[0, 0]).wait_recv()
    for d in order:
        col_copy(d).wait_recv()
        col_copy(d).wait_send()
        ep_copy(d).wait_send()
    for s in range(chips):
        shard_step(s, waiting=True)
    for d in steps:
        for via in (1, 2) if relay else range(1, tp_count):
            for h in range(len(halves)):
                tp_copy(0, d, via, h).wait_send()
        if relay:
            tp_copy(1, d, 2, 0).wait_send()
            tp_copy(2, d, 1, 1).wait_send()


def dispatch(sent, grads, cols, ep_count, tp_count, width):
    halves = 2 if tp_count == 4 else 1
    dma = pltpu.SemaphoreType.DMA
    vmem = pl.BlockSpec(memory_space=pltpu.VMEM)
    return pl.pallas_call(
        functools.partial(dispatch_kernel, ep_count, tp_count, width),
        out_shape=[
            jax.ShapeDtypeStruct((tp_count,) + sent.shape, sent.dtype),
            jax.ShapeDtypeStruct((ep_count,) + grads.shape, grads.dtype),
            jax.ShapeDtypeStruct(cols.shape, cols.dtype),
        ],
        in_specs=[vmem] * 3,
        out_specs=[vmem] * 3,
        scratch_shapes=[
            dma((ep_count,)), dma((ep_count,)),
            dma((tp_count, ep_count, halves)), dma((tp_count, ep_count, halves)),
            dma((ep_count,)), dma((ep_count,)),
            dma((ep_count,)), dma((ep_count,)), dma((2, ep_count)), dma((ep_count,)),
        ],
        compiler_params=pltpu.CompilerParams(
            collective_id=0, has_side_effects=True, vmem_limit_bytes=40 * 1024 * 1024
        ),
        name="dispatch",
    )(sent, grads, cols)


def combine_kernel(
    ep_count, tp_count, width, blocks, out, parts, reduced, tp_send, tp_recv, ep_send, ep_recv
):
    me, mine = lax.axis_index("ep"), lax.axis_index("tp")
    greet(me, ep_count, mine, tp_count)
    order = list(range(ep_count - 1, -1, -1))

    def tp_copy(d, via):
        return remote(
            blocks.at[mine ^ via, me ^ d],
            parts.at[via, d],
            tp_send.at[via, d],
            tp_recv.at[via, d],
            (me, mine ^ via),
        )

    def ep_copy(d):
        return remote(reduced.at[d], out.at[me], ep_send.at[d], ep_recv.at[d], (me ^ d, mine))

    for d in order:
        for via in range(1, tp_count):
            tp_copy(d, via).start()
    for d in order:
        for via in range(1, tp_count):
            tp_copy(d, via).wait_recv()
        whole = blocks[mine, me ^ d].astype(jnp.float32)
        for via in range(1, tp_count):
            whole = whole + parts[via, d].astype(jnp.float32)
        high = whole.astype(jnp.bfloat16)
        side = whole[:, width:]
        low = (side - high[:, width:].astype(jnp.float32)).astype(jnp.bfloat16)
        if d:
            reduced[d, :, : width + LANES] = high
            reduced[d, :, width + LANES :] = low
            ep_copy(d).start()
        else:
            out[me, :, : width + LANES] = high
            out[me, :, width + LANES :] = low
    for d in order:
        for via in range(1, tp_count):
            tp_copy(d, via).wait_send()
        if d:
            ep_copy(d).wait_recv()
            ep_copy(d).wait_send()


def combine(blocks, ep_count, tp_count, width):
    rows = blocks.shape[2]
    dma = pltpu.SemaphoreType.DMA
    vmem = pl.BlockSpec(memory_space=pltpu.VMEM)
    final = (ep_count, rows, width + 2 * LANES)
    return pl.pallas_call(
        functools.partial(combine_kernel, ep_count, tp_count, width),
        out_shape=jax.ShapeDtypeStruct(final, blocks.dtype),
        in_specs=[vmem],
        out_specs=vmem,
        scratch_shapes=[
            pltpu.VMEM(blocks.shape, blocks.dtype),
            pltpu.VMEM(final, blocks.dtype),
            dma((tp_count, ep_count)), dma((tp_count, ep_count)),
            dma((ep_count,)), dma((ep_count,)),
        ],
        compiler_params=pltpu.CompilerParams(
            collective_id=1, has_side_effects=True, vmem_limit_bytes=40 * 1024 * 1024
        ),
        name="combine",
    )(blocks)


def slot_masks(routes, num_experts, capacity):
    tok_rows, per_token = routes.shape
    expert_ids = lax.broadcasted_iota(jnp.int32, (tok_rows, num_experts), 1)
    chosen = [routes[:, k : k + 1] == expert_ids for k in range(per_token)]
    named = sum(c.astype(jnp.bfloat16) for c in chosen)
    before = (
        lax.broadcasted_iota(jnp.int32, (tok_rows, tok_rows), 1)
        < lax.broadcasted_iota(jnp.int32, (tok_rows, tok_rows), 0)
    ).astype(jnp.bfloat16)
    rank = jnp.dot(before, named, preferred_element_type=jnp.float32)
    slots = lax.broadcasted_iota(jnp.int32, (num_experts * capacity, tok_rows), 0)
    masks = []
    for k in range(per_token):
        own_rank = jnp.sum(jnp.where(chosen[k], rank, 0.0), axis=1).astype(jnp.int32)
        masks.append(slots == (routes[:, k] * capacity + own_rank)[None, :])
    return masks


def split_columns(values, width):
    rounded = lax.reduce_precision(values, 8, 7)
    high = rounded.astype(jnp.bfloat16)
    low = (values - rounded).astype(jnp.bfloat16)
    pair = jnp.stack([high, low], axis=-1)
    return jnp.pad(pair, [(0, 0)] * values.ndim + [(0, width - 2)])


def local(tokens, out_grad, routes, route_weights, gate_proj, up_proj, down_proj, shared_hidden):
    ep_count = lax.axis_size("ep")
    tp_count = lax.axis_size("tp")
    local_experts = gate_proj.shape[0]
    num_experts = local_experts * ep_count
    tok_rows, per_token = routes.shape
    width = tokens.shape[1]
    capacity = max(2, 5 * tok_rows * per_token // (4 * num_experts))
    slot_count = num_experts * capacity
    masks = slot_masks(routes, num_experts, capacity)
    picks = [m.astype(jnp.bfloat16) for m in masks]
    pick = sum(picks)
    weight_b = route_weights.astype(jnp.bfloat16).astype(jnp.float32)
    slot_weight = sum(
        jnp.sum(jnp.where(masks[k], weight_b[:, k][None, :], 0.0), axis=1)
        for k in range(per_token)
    ).astype(jnp.bfloat16)
    sent = jnp.concatenate(
        [
            jnp.dot(pick, tokens, preferred_element_type=jnp.float32).astype(jnp.bfloat16),
            jnp.dot(pick, out_grad, preferred_element_type=jnp.float32).astype(jnp.bfloat16),
            jnp.pad(slot_weight[:, None], ((0, 0), (0, LANES - 1))),
        ],
        axis=1,
    ).reshape(ep_count, local_experts * capacity, 2 * width + LANES)
    cols = shared_hidden.reshape(tok_rows, ep_count, -1).transpose(1, 0, 2)
    full, all_grads, all_cols = dispatch(sent, out_grad, cols, ep_count, tp_count, width)

    def features(part):
        part = part.reshape(tp_count, ep_count, local_experts, capacity, width)
        part = part.transpose(2, 1, 3, 0, 4)
        return part.reshape(local_experts, ep_count * capacity, tp_count * width)

    rows_in = features(full[..., :width])
    grads_in = features(full[..., width : 2 * width])
    scales = full[0, :, :, 2 * width].reshape(ep_count, local_experts, capacity)
    slot_scale = scales.transpose(1, 0, 2).reshape(local_experts, -1).astype(jnp.float32)
    pre_gate = jnp.einsum("lrd,lfd->lrf", rows_in, gate_proj, preferred_element_type=jnp.float32)
    pre_up = jnp.einsum("lrd,lfd->lrf", rows_in, up_proj, preferred_element_type=jnp.float32)
    squash = jax.nn.sigmoid(pre_gate)
    activated = pre_gate * squash
    hidden = (activated * pre_up).astype(jnp.bfloat16)
    back_grad = jnp.einsum("lrd,lfd->lrf", grads_in, down_proj, preferred_element_type=jnp.float32)
    products = jnp.sum(hidden.astype(jnp.float32) * back_grad, axis=2)
    hidden_grad = slot_scale[:, :, None] * back_grad
    scaled_hidden = (slot_scale[:, :, None] * hidden.astype(jnp.float32)).astype(jnp.bfloat16)
    gate_delta = (hidden_grad * pre_up * squash * (1.0 + pre_gate * (1.0 - squash))).astype(
        jnp.bfloat16
    )
    up_delta = (hidden_grad * activated).astype(jnp.bfloat16)
    sides = split_columns(products, LANES)
    blocks = []
    for t in range(tp_count):
        cut = slice(t * width, (t + 1) * width)
        part = jnp.einsum(
            "lrf,lfd->lrd", gate_delta, gate_proj[:, :, cut], preferred_element_type=jnp.float32
        ) + jnp.einsum(
            "lrf,lfd->lrd", up_delta, up_proj[:, :, cut], preferred_element_type=jnp.float32
        )
        blocks.append(jnp.concatenate([part.astype(jnp.bfloat16), sides], axis=2))
    blocks = jnp.stack(blocks).reshape(tp_count, local_experts, ep_count, capacity, -1)
    blocks = blocks.transpose(0, 2, 1, 3, 4)
    blocks = blocks.reshape(tp_count, ep_count, local_experts * capacity, -1)
    slot_rows = combine(blocks, ep_count, tp_count, width).reshape(slot_count, -1)
    gate_grad = jnp.einsum(
        "lrf,lrd->lfd", gate_delta, rows_in, preferred_element_type=jnp.float32
    ).astype(jnp.bfloat16)
    up_grad = jnp.einsum(
        "lrf,lrd->lfd", up_delta, rows_in, preferred_element_type=jnp.float32
    ).astype(jnp.bfloat16)
    down_grad = jnp.einsum(
        "lrf,lrd->lfd", scaled_hidden, grads_in, preferred_element_type=jnp.float32
    ).astype(jnp.bfloat16)
    contract_slots = (((0,), (0,)), ((), ()))
    token_grad = lax.dot_general(
        pick, slot_rows[:, :width], contract_slots, preferred_element_type=jnp.float32
    ).astype(jnp.bfloat16)
    tail = slot_rows[:, width:].astype(jnp.float32)
    slot_product = tail[:, 0] + tail[:, 1] + tail[:, LANES] + tail[:, LANES + 1]
    slot_product = slot_product[:, None]
    weight_grad = jnp.stack(
        [jnp.sum(jnp.where(m, slot_product, 0.0), axis=0) for m in masks], axis=1
    )
    shared_grad = jnp.einsum(
        "jth,jtd->hd", all_cols, all_grads, preferred_element_type=jnp.float32
    )
    return (token_grad, weight_grad, gate_grad, up_grad, down_grad, shared_grad)


def solution(mesh):
    return jax.shard_map(
        local,
        mesh=mesh,
        in_specs=(
            P("ep", "tp"),
            P("ep", "tp"),
            P("ep", None),
            P("ep", None),
            P("ep", "tp", None),
            P("ep", "tp", None),
            P("ep", "tp", None),
            P("ep", None),
        ),
        out_specs=(
            P("ep", "tp"),
            P("ep", None),
            P("ep", "tp", None),
            P("ep", "tp", None),
            P("ep", "tp", None),
            P("ep", "tp"),
        ),
        check_vma=False,
    )
```
